32 devices in a mesh: sp: 4 (over z), dp: 8 (over y, x, core).
Axes of the slice: x: 2, y: 2, z: 4, core: 2. Of those that a mesh axis runs over, the one named last changes fastest.
Arguments:
- queries: bfloat16 [8, 512, 1024], P('dp', 'sp'), may hold values from -300 to 300
- keys: bfloat16 [8, 512, 1024], P('dp', 'sp'), may hold values from -7 to 7
- values: bfloat16 [8, 512, 1024], P('dp', 'sp'), may hold values from -6 to 6
- cum_gates: float32 [8, 16, 512], P('dp', 'sp'), may hold values from -67 to 0, as said below
- out_weight: bfloat16 [1024, 2048], P(None, 'dp'), may hold values from -0.1875 to 0.1875
Outputs:
- mixed: bfloat16 [8, 512, 2048], P('dp', 'sp')
The draws below stay inside these ranges and needn't reach their ends.
Inputs may be any that keep to these rules, and one draw needn't show every extreme that they name: `cum_gates`: never rises along positions.
All inputs are finite; a program needn't handle non-finite values.
Results may differ from the reference program's by a relative error of at most 0.011.
Values may be sent and summed in bfloat16 or wider, within the bound.
A program may use at most 64 MiB of HBM per device.

```python
import jax
import jax.numpy as jnp
from jax import lax

D = 2048
HEAD_TOTAL = 16
HEAD_DIM = 64
TOK_DEV = 128
SEQUENCE_LENGTH = 512
SEQUENCE_COUNT = 8


def make_pair(key):
    width = HEAD_TOTAL * HEAD_DIM
    queries = jnp.clip(jax.random.normal(jax.random.fold_in(key, 11), (SEQUENCE_COUNT, SEQUENCE_LENGTH, width), jnp.float32), -6.0, 6.0)
    keys = jnp.clip(jax.random.normal(jax.random.fold_in(key, 12), (SEQUENCE_COUNT, SEQUENCE_LENGTH, width), jnp.float32), -6.0, 6.0)
    return (queries, keys)


def draw_queries(key, part):
    return make_pair(key)[0].astype(jnp.bfloat16)


def draw_keys(key, part):
    return make_pair(key)[1].astype(jnp.bfloat16)


def draw_cum_gates(key, part):
    token_position = jnp.arange(SEQUENCE_LENGTH)
    order = jax.random.permutation(jax.random.fold_in(key, 21), HEAD_TOTAL)
    slow_mask = jnp.broadcast_to((order < HEAD_TOTAL // 2)[None, :, None], (SEQUENCE_COUNT, HEAD_TOTAL, 1))
    slow_rate = jax.random.uniform(jax.random.fold_in(key, 22), (SEQUENCE_COUNT, HEAD_TOTAL, 1), jnp.float32, 0.3, 1.0) / SEQUENCE_LENGTH
    fast_rate = jnp.exp(jax.random.uniform(jax.random.fold_in(key, 23), (SEQUENCE_COUNT, HEAD_TOTAL, 1), jnp.float32, jnp.log(1.0 / 100.0), jnp.log(1.0 / 30.0)))
    rate = jnp.where(slow_mask, slow_rate, fast_rate)
    block_count = SEQUENCE_LENGTH // TOK_DEV
    block_factor = jnp.exp(jax.random.uniform(jax.random.fold_in(key, 24), (SEQUENCE_COUNT, 1, block_count), jnp.float32, jnp.log(0.5), jnp.log(2.0)))
    factor = block_factor[:, :, token_position // TOK_DEV]
    rough = jax.random.uniform(jax.random.fold_in(key, 25), (SEQUENCE_COUNT, HEAD_TOTAL, SEQUENCE_LENGTH), jnp.float32, 0.3, 1.7)
    logarithm_gate = -rate * factor * rough
    spike_location = jax.random.randint(jax.random.fold_in(key, 26), (SEQUENCE_COUNT, HEAD_TOTAL, 3), 0, SEQUENCE_LENGTH)
    spike_decrease = jax.random.uniform(jax.random.fold_in(key, 27), (SEQUENCE_COUNT, HEAD_TOTAL, 3), jnp.float32, 0.2, 0.5)
    match_count = (token_position[None, None, None, :] == spike_location[:, :, :, None]).astype(jnp.float32)
    spike_events = jnp.sum(match_count * jnp.log(1.0 - spike_decrease)[:, :, :, None], axis=2)
    return jnp.cumsum(logarithm_gate + spike_events, axis=-1).astype(jnp.float32)


def level_of(rng, extent, pieces, smallest, largest):
    loudness = 1.0
    for position, parts in pieces:
        draws = jax.random.uniform(jax.random.fold_in(jax.random.fold_in(rng, 6), position), (parts,), jnp.float32, smallest / len(pieces), largest / len(pieces))
        loudness = loudness * jnp.repeat(jnp.exp(draws), extent[position] // parts).reshape((-1,) + (1,) * (len(extent) - 1 - position))
    return loudness


def gaussian(rng, dims, spread, limit, split=(), dtype=jnp.bfloat16):
    entries = spread * jax.random.normal(rng, dims, jnp.float32)
    if split:
        entries = entries * level_of(rng, dims, split, -0.22, 0.18)
    return jnp.clip(entries, -limit, limit).astype(dtype)


def setup_inputs(seed: int = 0) -> dict:
    arg_keys = jax.random.split(jax.random.key(seed), 6)
    return {
        "queries": draw_queries(jax.random.fold_in(arg_keys[5], 71), 0),
        "keys": draw_keys(jax.random.fold_in(arg_keys[5], 71), 0),
        "values": gaussian(arg_keys[2], (SEQUENCE_COUNT, SEQUENCE_LENGTH, HEAD_TOTAL * HEAD_DIM), 1.0, 6.0, ((0, 8), (1, 4))),
        "cum_gates": draw_cum_gates(jax.random.fold_in(arg_keys[5], 71), 0),
        "out_weight": gaussian(arg_keys[4], (HEAD_TOTAL * HEAD_DIM, D), (HEAD_TOTAL * HEAD_DIM) ** -0.5, 0.1875, ((1, 8),)),
    }


def attend_sequence(packed, out_weight):
    query_rows, key_rows, value_rows, cum_rows = packed
    length = query_rows.shape[0]
    head_count = cum_rows.shape[0]
    head_size = query_rows.shape[1] // head_count
    query_heads = query_rows.astype(jnp.float32).reshape(length, head_count, head_size).transpose(1, 0, 2)
    key_heads = key_rows.astype(jnp.float32).reshape(length, head_count, head_size).transpose(1, 0, 2)
    value_heads = value_rows.astype(jnp.float32).reshape(length, head_count, head_size).transpose(1, 0, 2)
    scores = jnp.einsum('hqd,hkd->hqk', query_heads, key_heads) * (head_size ** -0.5)
    scores = scores + cum_rows[:, :, None] - cum_rows[:, None, :]
    token_position = jnp.arange(length)
    scores = jnp.where(token_position[None, :] <= token_position[:, None], scores, -jnp.inf)
    row_max = jnp.max(scores, axis=-1, keepdims=True)
    expon = jnp.exp(scores - row_max)
    weights = (expon / jnp.sum(expon, axis=-1, keepdims=True)).astype(jnp.bfloat16)
    head_out = jnp.einsum('hqk,hkd->hqd', weights.astype(jnp.float32), value_heads).astype(jnp.bfloat16)
    head_out = head_out.transpose(1, 0, 2).reshape(length, head_count * head_size)
    return jnp.dot(head_out, out_weight, preferred_element_type=jnp.float32).astype(jnp.bfloat16)


def reference(queries, keys, values, cum_gates, out_weight):
    return lax.map(lambda packed: attend_sequence(packed, out_weight), (queries, keys, values, cum_gates))
```

```python
import functools

import jax
import jax.numpy as jnp
from jax import lax
from jax.experimental import pallas as pl
from jax.experimental.pallas import tpu as pltpu
from jax.sharding import PartitionSpec as P


def attend_heads(query_loc, key_loc, value_loc, cum_loc):
    length = query_loc.shape[0]
    head_count = cum_loc.shape[0]
    head_size = query_loc.shape[1] // head_count
    query_heads = query_loc.reshape(length, head_count, head_size).transpose(1, 0, 2)
    key_heads = key_loc.reshape(length, head_count, head_size).transpose(1, 0, 2)
    value_heads = value_loc.reshape(length, head_count, head_size).transpose(1, 0, 2)
    block_rows = min(512, length)
    block_count = length // block_rows
    query_blocks = query_heads.reshape(head_count, block_count, block_rows, head_size).transpose(
        1, 0, 2, 3
    )
    cum_blocks = cum_loc.reshape(head_count, block_count, block_rows).transpose(1, 0, 2)
    key_pos = jnp.arange(length)
    score_scale = head_size ** (-0.5)

    def one_block(packed):
        query_block, cum_block, block_index = packed
        scores = (
            jnp.einsum("hqd,hkd->hqk", query_block, key_heads, preferred_element_type=jnp.float32)
            * score_scale
        )
        scores = scores + cum_block[:, :, None] - cum_loc[:, None, :]
        query_pos = block_index * block_rows + jnp.arange(block_rows)
        scores = jnp.where(key_pos[None, :] <= query_pos[:, None], scores, -jnp.inf)
        row_max = jnp.max(scores, axis=-1, keepdims=True)
        expon = jnp.exp(scores - row_max)
        weights = (expon / jnp.sum(expon, axis=-1, keepdims=True)).astype(jnp.bfloat16)
        return jnp.einsum(
            "hqk,hkd->hqd", weights, value_heads, preferred_element_type=jnp.float32
        ).astype(jnp.bfloat16)

    results = lax.map(one_block, (query_blocks, cum_blocks, jnp.arange(block_count)))
    return results.transpose(0, 2, 1, 3).reshape(length, head_count * head_size)


def shards(queries, keys, values, cum_gates, out_weight):
    query_loc, key_loc, value_loc = (
        lax.all_to_all(queries[0], "sp", split_axis=1, concat_axis=0, tiled=True),
        lax.all_to_all(keys[0], "sp", split_axis=1, concat_axis=0, tiled=True),
        lax.all_to_all(values[0], "sp", split_axis=1, concat_axis=0, tiled=True),
    )
    head_out = attend_heads(query_loc, key_loc, value_loc, cum_gates[0])
    token_rows = lax.all_to_all(head_out, "sp", split_axis=0, concat_axis=1, tiled=True)
    mixed_rows = jnp.dot(
        token_rows,
        lax.all_gather(out_weight, "dp", axis=1, tiled=True),
        preferred_element_type=jnp.float32,
    )
    return mixed_rows.astype(jnp.bfloat16)[None]


MESH = pl.DeviceIdType.MESH
LANES = 128
HUB = 1


def flip(index, bit):
    return index + bit - 2 * bit * (lax.div(index, bit) % 2)


def head_pair(q, ks, vs, gates, first_key, row_block, scale, head_size, causal):
    rows = q.shape[0]
    even = lax.broadcasted_iota(jnp.int32, (rows, LANES), 1) < head_size
    q = q * jnp.asarray(scale, q.dtype)
    zero = jnp.zeros_like(q)
    stacked = jnp.concatenate([jnp.where(even, q, zero), jnp.where(even, zero, q)], axis=0)
    k = ks[0] if len(ks) == 1 else jnp.concatenate(ks, axis=0)
    v = vs[0] if len(vs) == 1 else jnp.concatenate(vs, axis=0)
    span = k.shape[0]
    scores = lax.dot_general(
        stacked, k, (((1,), (1,)), ((), ())), preferred_element_type=jnp.float32
    )
    key_gates = gates[:, pl.ds(pl.multiple_of(first_key * rows, LANES), span)]
    row_gates = gates[:, pl.ds(pl.multiple_of(row_block * rows, LANES), rows)].T
    parts = []
    for n in range(2):
        part = scores[n * rows : (n + 1) * rows] + (
            row_gates[:, 8 * n : 8 * n + 1] - key_gates[8 * n : 8 * n + 1]
        )
        if causal:
            row = lax.broadcasted_iota(jnp.int32, (rows, span), 0) + (span - rows)
            col = lax.broadcasted_iota(jnp.int32, (rows, span), 1)
            part = jnp.where(col <= row, part, -jnp.inf)
        parts.append(part)
    tops = [jnp.max(part, axis=1, keepdims=True) for part in parts]
    probs = jnp.concatenate(
        [jnp.exp(part - top).astype(v.dtype) for part, top in zip(parts, tops)], axis=0
    )
    wide = jnp.concatenate([v, jnp.ones((span, LANES), v.dtype)], axis=1)
    sums = jnp.dot(probs, wide, preferred_element_type=jnp.float32)
    total = jnp.where(even, sums[:rows, LANES:], sums[rows:, LANES:])
    result = jnp.where(even, sums[:rows, :LANES], sums[rows:, :LANES]) / total
    top = jnp.where(even, tops[0], tops[1])
    return result, top + jnp.log(total)


def layer_kernel(
    sizes, q_hbm, k_hbm, v_hbm, g_hbm, w_hbm, out_ref,
    q_own, q_in, k_buf, v_buf, g_in, g_pair, o_out, s_out, o_in, s_in, o_own, s_own, heads, w_buf,
    q_ss, q_rs, kv_ss, kv_rs, o_ss, o_rs, s_ss, s_rs, g_ss, g_rs, w_ss, w_rs, loc,
):
    sp, chunks, head_size, scale = sizes
    z, d = lax.axis_index("sp"), lax.axis_index("dp")
    rows = q_own.shape[0]
    half = w_buf.shape[1] // 2
    core, xs, ys = flip(d, 1), flip(d, 2), flip(d, 4)

    def cols(c):
        return pl.ds(pl.multiple_of(c * LANES, LANES), LANES)

    def remote(src, dst, ss, rs, **device):
        return pltpu.make_async_remote_copy(
            src_ref=src, dst_ref=dst, send_sem=ss, recv_sem=rs,
            device_id=device, device_id_type=MESH,
        )

    local = [
        pltpu.make_async_copy(q_hbm.at[0], q_own, loc.at[0]),
        pltpu.make_async_copy(k_hbm.at[0], k_buf.at[1], loc.at[1]),
        pltpu.make_async_copy(v_hbm.at[0], v_buf.at[1], loc.at[2]),
        pltpu.make_async_copy(g_hbm.at[0], g_in.at[z], loc.at[3]),
        pltpu.make_async_copy(w_hbm, w_buf.at[0], loc.at[4]),
    ]
    for copy in local:
        copy.start()

    barrier = pltpu.get_barrier_semaphore()
    for step in range(1, sp):
        pl.semaphore_signal(
            barrier, inc=1, device_id={"sp": lax.rem(z + step, sp)}, device_id_type=MESH
        )
    for peer in (core, xs, ys):
        pl.semaphore_signal(barrier, inc=1, device_id={"dp": peer}, device_id_type=MESH)
    pl.semaphore_wait(barrier, sp - 1 + 3)

    def gate_copy(step):
        return remote(
            g_hbm.at[0], g_in.at[z], g_ss.at[step], g_rs.at[z], sp=lax.rem(z + step, sp)
        )

    for step in range(1, sp):
        gate_copy(step).start()

    def q_copy(c, slot, way, target):
        return remote(
            q_hbm.at[0, :, cols(c)], q_in.at[slot, :, cols(c)],
            q_ss.at[way, c], q_rs.at[slot, c], sp=target,
        )

    def k_copy(c):
        return remote(
            k_hbm.at[0, :, cols(c)], k_buf.at[0, :, cols(c)],
            kv_ss.at[0, c], kv_rs.at[0, c], sp=HUB,
        )

    def v_copy(c):
        return remote(
            v_hbm.at[0, :, cols(c)], v_buf.at[0, :, cols(c)],
            kv_ss.at[1, c], kv_rs.at[1, c], sp=HUB,
        )

    @pl.when(z == 0)
    def _():
        for c in range(chunks):
            k_copy(c).start()
            v_copy(c).start()

    @pl.when(z == HUB + 1)
    def _():
        for c in range(chunks):
            q_copy(c, 0, 0, HUB).start()

    @pl.when(z == HUB + 2)
    def _():
        for c in range(chunks):
            q_copy(c, 1, 0, HUB).start()
            q_copy(c, 1, 1, HUB + 1).start()

    def w_copy(number, slot, part, bit, peer):
        span = pl.ds(part * half, half)
        src = w_hbm.at[span] if slot == 0 else w_buf.at[slot, span]
        return remote(
            src, w_buf.at[slot ^ bit, span], w_ss.at[number], w_rs.at[slot ^ bit, part], dp=peer
        )

    w_plan = {
        "first": [(0, 0, 0, 2, xs), (1, 0, 1, 4, ys), (2, 0, 1, 2, xs), (3, 0, 0, 4, ys),
                  (4, 0, 0, 1, core), (5, 0, 1, 1, core)],
        "early": [(6, 2, 0, 4, ys), (7, 4, 1, 2, xs), (8, 2, 0, 1, core), (9, 4, 1, 1, core)],
        "middle": [(10, 2, 1, 1, core), (11, 4, 0, 1, core)],
        "late": [(12, 6, 0, 1, core), (13, 6, 1, 1, core)],
    }

    def w_arrived(slot, part):
        span = pl.ds(part * half, half)
        remote(
            w_hbm.at[span], w_buf.at[slot, span], w_ss.at[0], w_rs.at[slot, part], dp=core
        ).wait_recv()

    def relay(stage):
        seen = []
        for number, slot, part, bit, peer in w_plan[stage]:
            if slot and (slot, part) not in seen:
                w_arrived(slot, part)
                seen.append((slot, part))
            w_copy(number, slot, part, bit, peer).start()

    relay("first")

    local[3].wait()
    for owner in range(sp):
        @pl.when(z != owner)
        def _():
            remote(
                g_hbm.at[0], g_in.at[owner], g_ss.at[0], g_rs.at[owner], sp=lax.rem(z + 1, sp)
            ).wait_recv()
    per = g_in.shape[1]
    for c in range(chunks):
        for n in range(2):
            head = 2 * c + n
            line = g_in[head // per, head % per : head % per + 1, :]
            g_pair[c, 8 * n : 8 * n + 8, :] = jnp.broadcast_to(line, (8, line.shape[1]))
    for copy in local[:3]:
        copy.wait()

    def attend(c, q, slots, first_key, row_block, causal):
        return head_pair(
            q[:, cols(c)], [k_buf[s, :, cols(c)] for s in slots],
            [v_buf[s, :, cols(c)] for s in slots],
            g_pair.at[c], first_key, row_block, scale, head_size, causal,
        )

    def put(c, slot, result, lse):
        o_out[slot, :, cols(c)] = result.astype(o_out.dtype)
        turned = lse.T
        s_out[slot, c, 0:8, :] = turned[0:8]
        s_out[slot, c, 8:16, :] = turned[head_size : head_size + 8]

    def o_copy(c, slot, into, target):
        return remote(
            o_out.at[slot, :, cols(c)], o_in.at[into, :, cols(c)],
            o_ss.at[slot, c], o_rs.at[into, c], sp=target,
        )

    def s_copy(c, slot, into, target):
        return remote(
            s_out.at[slot, c], s_in.at[into, c], s_ss.at[slot, c], s_rs.at[into, c], sp=target
        )

    def give(c, slot, into, target):
        s_copy(c, slot, into, target).start()
        o_copy(c, slot, into, target).start()

    def early(c):
        @pl.when(c == chunks // 2)
        def _():
            relay("early")

    @pl.when(z == 0)
    def _():
        @pl.loop(0, chunks)
        def _(c):
            early(c)
            result, _lse = attend(c, q_own, [1], z, z, True)
            heads[:, cols(c)] = result.astype(heads.dtype)

    @pl.when(z == HUB)
    def _():
        @pl.loop(0, chunks)
        def _(c):
            early(c)
            k_copy(c).wait_recv()
            v_copy(c).wait_recv()
            q_copy(c, 1, 0, HUB).wait_recv()
            put(c, 1, *attend(c, q_in.at[1], [0, 1], 0, HUB + 2, False))
            q_copy(c, 0, 0, HUB).wait_recv()
            put(c, 0, *attend(c, q_in.at[0], [0, 1], 0, HUB + 1, False))
            give(c, 1, 0, HUB + 2)
            result, _lse = attend(c, q_own, [0, 1], 0, z, True)
            heads[:, cols(c)] = result.astype(heads.dtype)
            give(c, 0, 0, HUB + 1)

    @pl.when(z > HUB)
    def _():
        @pl.loop(0, chunks)
        def _(c):
            early(c)

            @pl.when(z == HUB + 1)
            def _():
                q_copy(c, 1, 1, HUB + 1).wait_recv()
                put(c, 1, *attend(c, q_in.at[1], [1], z, HUB + 2, False))

            result, lse = attend(c, q_own, [1], z, z, True)
            o_own[:, cols(c)] = result
            s_own[:, cols(c)] = lse

            @pl.when(z == HUB + 1)
            def _():
                give(c, 1, 1, HUB + 2)

    def taken(c, into):
        s_copy(c, 0, into, HUB).wait_recv()
        o_copy(c, 0, into, HUB).wait_recv()
        turned = s_in[into, c].T
        even = lax.broadcasted_iota(jnp.int32, (rows, LANES), 1) < head_size
        lse = jnp.where(even, turned[:, 0:1], turned[:, 8:9])
        return o_in[into, :, cols(c)].astype(jnp.float32), lse

    def merge(first, second):
        (a, la), (b, lb) = first, second
        top = jnp.maximum(la, lb)
        wa, wb = jnp.exp(la - top), jnp.exp(lb - top)
        total = wa + wb
        return (a * wa + b * wb) / total, top + jnp.log(total)

    @pl.when(z <= HUB)
    def _():
        relay("middle")

    @pl.when(z > HUB)
    def _():
        @pl.loop(0, chunks)
        def _(c):
            @pl.when(c == chunks // 2 + 1)
            def _():
                relay("middle")

            @pl.when(z == HUB + 2)
            def _():
                result, lse = merge((o_own[:, cols(c)], s_own[:, cols(c)]), taken(c, 1))
                o_own[:, cols(c)] = result
                s_own[:, cols(c)] = lse

            result, _lse = merge((o_own[:, cols(c)], s_own[:, cols(c)]), taken(c, 0))
            heads[:, cols(c)] = result.astype(heads.dtype)

        relay("late")

    width = w_buf.shape[2]

    def project(slot):
        owner = d
        for bit in (1, 2, 4):
            if slot & bit:
                owner = flip(owner, bit)
        block = jnp.dot(heads[...], w_buf[slot], preferred_element_type=jnp.float32)
        out_ref[0, :, pl.ds(pl.multiple_of(owner * width, LANES), width)] = block.astype(
            out_ref.dtype
        )

    local[4].wait()
    project(0)
    for part in range(2):
        w_arrived(1, part)
    project(1)
    project(2)
    project(4)
    for slot in (3, 5):
        for part in range(2):
            w_arrived(slot, part)
        project(slot)

    @pl.when(z <= HUB)
    def _():
        relay("late")

    project(6)
    for part in range(2):
        w_arrived(7, part)
    project(7)

    for step in range(1, sp):
        gate_copy(step).wait_send()
    for stage in w_plan.values():
        for entry in stage:
            w_copy(*entry).wait_send()

    @pl.when(z == 0)
    def _():
        for c in range(chunks):
            k_copy(c).wait_send()
            v_copy(c).wait_send()

    @pl.when(z > HUB)
    def _():
        for c in range(chunks):
            q_copy(c, 0, 0, HUB).wait_send()

    @pl.when(z == HUB + 2)
    def _():
        for c in range(chunks):
            q_copy(c, 1, 1, HUB + 1).wait_send()

    @pl.when((z == HUB) | (z == HUB + 1))
    def _():
        for c in range(chunks):
            s_copy(c, 1, 0, HUB + 2).wait_send()
            o_copy(c, 1, 0, HUB + 2).wait_send()

    @pl.when(z == HUB)
    def _():
        for c in range(chunks):
            s_copy(c, 0, 0, HUB + 1).wait_send()
            o_copy(c, 0, 0, HUB + 1).wait_send()


def fused_shards(sp, queries, keys, values, cum_gates, out_weight):
    _, rows, width = queries.shape
    _, per, length = cum_gates.shape
    head_size = width // (per * sp)
    depth, block = out_weight.shape
    dp = 8
    chunks = width // LANES
    bf16, f32 = queries.dtype, jnp.float32
    dma = pltpu.SemaphoreType.DMA
    return pl.pallas_call(
        functools.partial(layer_kernel, (sp, chunks, head_size, head_size ** (-0.5))),
        out_shape=jax.ShapeDtypeStruct((1, rows, block * dp), bf16),
        in_specs=[pl.BlockSpec(memory_space=pl.ANY)] * 5,
        out_specs=pl.BlockSpec(memory_space=pltpu.VMEM),
        scratch_shapes=[
            pltpu.VMEM((rows, width), bf16),
            pltpu.VMEM((2, rows, width), bf16),
            pltpu.VMEM((2, rows, width), bf16),
            pltpu.VMEM((2, rows, width), bf16),
            pltpu.VMEM((sp, per, length), f32),
            pltpu.VMEM((chunks, 16, length), f32),
            pltpu.VMEM((2, rows, width), bf16),
            pltpu.VMEM((2, chunks, 16, LANES), f32),
            pltpu.VMEM((2, rows, width), bf16),
            pltpu.VMEM((2, chunks, 16, LANES), f32),
            pltpu.VMEM((rows, width), f32),
            pltpu.VMEM((rows, width), f32),
            pltpu.VMEM((rows, width), bf16),
            pltpu.VMEM((dp, depth, block), bf16),
            dma((2, chunks)), dma((2, chunks)), dma((2, chunks)), dma((2, chunks)),
            dma((2, chunks)), dma((2, chunks)), dma((2, chunks)), dma((2, chunks)),
            dma((sp,)), dma((sp,)), dma((14,)), dma((dp, 2)), dma((5,)),
        ],
        compiler_params=pltpu.CompilerParams(collective_id=0, has_side_effects=True),
        name="layer",
    )(queries, keys, values, cum_gates, out_weight)


def route(sp, dp, queries, keys, values, cum_gates, out_weight):
    _, rows, width = queries.shape
    head_size = width // (cum_gates.shape[1] * sp)
    fits = (
        sp == HUB + 3
        and dp == 8
        and rows == LANES
        and 2 * head_size == LANES
        and width % LANES == 0
        and out_weight.shape[1] % LANES == 0
    )
    if fits:
        return fused_shards(sp, queries, keys, values, cum_gates, out_weight)
    return shards(queries, keys, values, cum_gates, out_weight)


def solution(mesh):
    in_specs = (
        P("dp", "sp", None),
        P("dp", "sp", None),
        P("dp", "sp", None),
        P("dp", "sp", None),
        P(None, "dp"),
    )
    out_specs = P("dp", "sp", None)
    body = functools.partial(route, mesh.shape["sp"], mesh.shape["dp"])
    return jax.shard_map(body, mesh=mesh, in_specs=in_specs, out_specs=out_specs, check_vma=False)
```

```python
import functools

import jax
import jax.numpy as jnp
from jax import lax
from jax.experimental import pallas as pl
from jax.experimental.pallas import tpu as pltpu
from jax.sharding import PartitionSpec as P


def attend_heads(query_loc, key_loc, value_loc, cum_loc):
    length = query_loc.shape[0]
    head_count = cum_loc.shape[0]
    head_size = query_loc.shape[1] // head_count
    query_heads = query_loc.reshape(length, head_count, head_size).transpose(1, 0, 2)
    key_heads = key_loc.reshape(length, head_count, head_size).transpose(1, 0, 2)
    value_heads = value_loc.reshape(length, head_count, head_size).transpose(1, 0, 2)
    block_rows = min(512, length)
    block_count = length // block_rows
    query_blocks = query_heads.reshape(head_count, block_count, block_rows, head_size).transpose(
        1, 0, 2, 3
    )
    cum_blocks = cum_loc.reshape(head_count, block_count, block_rows).transpose(1, 0, 2)
    key_pos = jnp.arange(length)
    score_scale = head_size ** (-0.5)

    def one_block(packed):
        query_block, cum_block, block_index = packed
        scores = (
            jnp.einsum("hqd,hkd->hqk", query_block, key_heads, preferred_element_type=jnp.float32)
            * score_scale
        )
        scores = scores + cum_block[:, :, None] - cum_loc[:, None, :]
        query_pos = block_index * block_rows + jnp.arange(block_rows)
        scores = jnp.where(key_pos[None, :] <= query_pos[:, None], scores, -jnp.inf)
        row_max = jnp.max(scores, axis=-1, keepdims=True)
        expon = jnp.exp(scores - row_max)
        weights = (expon / jnp.sum(expon, axis=-1, keepdims=True)).astype(jnp.bfloat16)
        return jnp.einsum(
            "hqk,hkd->hqd", weights, value_heads, preferred_element_type=jnp.float32
        ).astype(jnp.bfloat16)

    results = lax.map(one_block, (query_blocks, cum_blocks, jnp.arange(block_count)))
    return results.transpose(0, 2, 1, 3).reshape(length, head_count * head_size)


def shards(queries, keys, values, cum_gates, out_weight):
    query_loc, key_loc, value_loc = (
        lax.all_to_all(queries[0], "sp", split_axis=1, concat_axis=0, tiled=True),
        lax.all_to_all(keys[0], "sp", split_axis=1, concat_axis=0, tiled=True),
        lax.all_to_all(values[0], "sp", split_axis=1, concat_axis=0, tiled=True),
    )
    head_out = attend_heads(query_loc, key_loc, value_loc, cum_gates[0])
    token_rows = lax.all_to_all(head_out, "sp", split_axis=0, concat_axis=1, tiled=True)
    mixed_rows = jnp.dot(
        token_rows,
        lax.all_gather(out_weight, "dp", axis=1, tiled=True),
        preferred_element_type=jnp.float32,
    )
    return mixed_rows.astype(jnp.bfloat16)[None]


MESH = pl.DeviceIdType.MESH
LANES = 128
HUB = 1


def flip(index, bit):
    return index + bit - 2 * bit * (lax.div(index, bit) % 2)


def head_pair(q, ks, vs, gates, first_key, row_block, scale, head_size, causal):
    rows = q.shape[0]
    even = lax.broadcasted_iota(jnp.int32, (rows, LANES), 1) < head_size
    q = q * jnp.asarray(scale, q.dtype)
    zero = jnp.zeros_like(q)
    stacked = jnp.concatenate([jnp.where(even, q, zero), jnp.where(even, zero, q)], axis=0)
    k = ks[0] if len(ks) == 1 else jnp.concatenate(ks, axis=0)
    v = vs[0] if len(vs) == 1 else jnp.concatenate(vs, axis=0)
    span = k.shape[0]
    scores = lax.dot_general(
        stacked, k, (((1,), (1,)), ((), ())), preferred_element_type=jnp.float32
    )
    key_gates = gates[:, pl.ds(pl.multiple_of(first_key * rows, LANES), span)]
    row_gates = gates[:, pl.ds(pl.multiple_of(row_block * rows, LANES), rows)].T
    parts = []
    for n in range(2):
        part = scores[n * rows : (n + 1) * rows] + (
            row_gates[:, 8 * n : 8 * n + 1] - key_gates[8 * n : 8 * n + 1]
        )
        if causal:
            row = lax.broadcasted_iota(jnp.int32, (rows, span), 0) + (span - rows)
            col = lax.broadcasted_iota(jnp.int32, (rows, span), 1)
            part = jnp.where(col <= row, part, -jnp.inf)
        parts.append(part)
    tops = [jnp.max(part, axis=1, keepdims=True) for part in parts]
    probs = jnp.concatenate(
        [jnp.exp(part - top).astype(v.dtype) for part, top in zip(parts, tops)], axis=0
    )
    wide = jnp.concatenate([v, jnp.ones((span, LANES), v.dtype)], axis=1)
    sums = jnp.dot(probs, wide, preferred_element_type=jnp.float32)
    total = jnp.where(even, sums[:rows, LANES:], sums[rows:, LANES:])
    result = jnp.where(even, sums[:rows, :LANES], sums[rows:, :LANES]) / total
    top = jnp.where(even, tops[0], tops[1])
    return result, top + jnp.log(total)


def layer_kernel(
    sizes, q_hbm, k_hbm, v_hbm, g_hbm, w_hbm, out_ref,
    q_own, q_in, k_buf, v_buf, g_in, g_pair, o_out, s_out, o_in, s_in, o_own, s_own, heads, w_buf,
    q_ss, q_rs, kv_ss, kv_rs, o_ss, o_rs, s_ss, s_rs, g_ss, g_rs, w_ss, w_rs, loc, seen_sem,
):
    sp, chunks, head_size, scale = sizes
    z, d = lax.axis_index("sp"), lax.axis_index("dp")
    rows = q_own.shape[0]
    half = w_buf.shape[1] // 2
    core, xs, ys = flip(d, 1), flip(d, 2), flip(d, 4)

    def cols(c):
        return pl.ds(pl.multiple_of(c * LANES, LANES), LANES)

    def remote(src, dst, ss, rs, **device):
        return pltpu.make_async_remote_copy(
            src_ref=src, dst_ref=dst, send_sem=ss, recv_sem=rs,
            device_id=device, device_id_type=MESH,
        )

    local = [
        pltpu.make_async_copy(q_hbm.at[0], q_own, loc.at[0]),
        pltpu.make_async_copy(k_hbm.at[0], k_buf.at[1], loc.at[1]),
        pltpu.make_async_copy(v_hbm.at[0], v_buf.at[1], loc.at[2]),
        pltpu.make_async_copy(g_hbm.at[0], g_in.at[z], loc.at[3]),
        pltpu.make_async_copy(w_hbm, w_buf.at[0], loc.at[4]),
    ]
    for copy in local:
        copy.start()

    barrier = pltpu.get_barrier_semaphore()
    @pl.when(z > 0)
    def _():
        pl.semaphore_signal(barrier, inc=1, device_id={"sp": z - 1}, device_id_type=MESH)

    @pl.when(z < sp - 1)
    def _():
        pl.semaphore_signal(barrier, inc=1, device_id={"sp": z + 1}, device_id_type=MESH)

    for peer in (core, xs, ys):
        pl.semaphore_signal(barrier, inc=1, device_id={"dp": peer}, device_id_type=MESH)
    pl.semaphore_wait(
        barrier, 3 + (z > 0).astype(jnp.int32) + (z < sp - 1).astype(jnp.int32)
    )

    for teller, pair in ((HUB + 1, (HUB, HUB + 2)), (HUB, (HUB - 1, HUB + 1))):
        @pl.when(z == teller)
        def _():
            for target in pair:
                pl.semaphore_signal(
                    seen_sem.at[teller - HUB], inc=1, device_id={"sp": target},
                    device_id_type=MESH,
                )

    def gate_copy(owner, target, relayed=0):
        return remote(
            g_in.at[owner], g_in.at[owner], g_ss.at[relayed, target], g_rs.at[owner], sp=target
        )

    def gate_sends(run):
        for owner, target in ((0, 1), (1, 0), (1, 2), (2, 1), (2, 3), (3, 2)):
            @pl.when(z == owner)
            def _():
                run(gate_copy(owner, target))

    def q_copy(c, slot, way, target):
        return remote(
            q_own.at[:, cols(c)], q_in.at[slot, :, cols(c)],
            q_ss.at[way, c], q_rs.at[slot, c], sp=target,
        )

    def k_copy(c):
        return remote(
            k_buf.at[1, :, cols(c)], k_buf.at[0, :, cols(c)],
            kv_ss.at[0, c], kv_rs.at[0, c], sp=HUB,
        )

    def v_copy(c):
        return remote(
            v_buf.at[1, :, cols(c)], v_buf.at[0, :, cols(c)],
            kv_ss.at[1, c], kv_rs.at[1, c], sp=HUB,
        )

    def w_copy(number, slot, part, bit, peer):
        span = pl.ds(part * half, half)
        return remote(
            w_buf.at[slot, span], w_buf.at[slot ^ bit, span], w_ss.at[number], w_rs.at[slot ^ bit, part], dp=peer
        )

    w_plan = {
        "first": [(0, 0, 0, 2, xs), (1, 0, 1, 4, ys), (2, 0, 1, 2, xs), (3, 0, 0, 4, ys),
                  (4, 0, 0, 1, core), (5, 0, 1, 1, core)],
        "early": [(6, 2, 0, 4, ys), (7, 4, 1, 2, xs), (8, 2, 0, 1, core), (9, 4, 1, 1, core)],
        "middle": [(10, 2, 1, 1, core), (11, 4, 0, 1, core)],
        "late": [(12, 6, 0, 1, core), (13, 6, 1, 1, core)],
    }

    def w_arrived(slot, part):
        span = pl.ds(part * half, half)
        remote(
            w_hbm.at[span], w_buf.at[slot, span], w_ss.at[0], w_rs.at[slot, part], dp=core
        ).wait_recv()

    def relay(stage):
        seen = []
        for number, slot, part, bit, peer in w_plan[stage]:
            if slot and (slot, part) not in seen:
                w_arrived(slot, part)
                seen.append((slot, part))
            w_copy(number, slot, part, bit, peer).start()

    local[4].wait()
    relay("first")
    for copy in local[:3]:
        copy.wait()

    local[3].wait()
    gate_sends(lambda copy: copy.start())

    @pl.when(z == 0)
    def _():
        for c in range(chunks):
            k_copy(c).start()
            v_copy(c).start()
            if c == 0:
                pl.semaphore_wait(seen_sem.at[0], 1)
                gate_copy(0, 2).start()

    @pl.when(z == HUB + 1)
    def _():
        for c in range(chunks):
            q_copy(c, 0, 0, HUB).start()
            if c == 0:
                pl.semaphore_wait(seen_sem.at[0], 1)
                gate_copy(2, 0).start()

    @pl.when(z == HUB + 2)
    def _():
        q_copy(0, 1, 1, HUB + 1).start()
        pl.semaphore_wait(seen_sem.at[1], 1)
        gate_copy(3, 1).start()
        q_copy(0, 1, 0, HUB).start()
        q_copy(1, 1, 0, HUB).start()
        for c in range(1, chunks):
            q_copy(c, 1, 1, HUB + 1).start()
            if c + 1 < chunks:
                q_copy(c + 1, 1, 0, HUB).start()

    @pl.when(z == HUB)
    def _():
        pl.semaphore_wait(seen_sem.at[1], 1)
        gate_copy(1, 3).start()

    for owner in range(sp):
        @pl.when(z != owner)
        def _():
            gate_copy(owner, (owner + 1) % sp).wait_recv()

    @pl.when(z == HUB)
    def _():
        gate_copy(0, 3, 1).start()
        gate_copy(3, 0, 1).start()

    per = g_in.shape[1]
    for c in range(chunks):
        for n in range(2):
            head = 2 * c + n
            line = g_in[head // per, head % per : head % per + 1, :]
            g_pair[c, 8 * n : 8 * n + 8, :] = jnp.broadcast_to(line, (8, line.shape[1]))
    def attend(c, q, slots, first_key, row_block, causal):
        return head_pair(
            q[:, cols(c)], [k_buf[s, :, cols(c)] for s in slots],
            [v_buf[s, :, cols(c)] for s in slots],
            g_pair.at[c], first_key, row_block, scale, head_size, causal,
        )

    def put(c, slot, result, lse):
        o_out[slot, :, cols(c)] = result.astype(o_out.dtype)
        turned = lse.T
        s_out[slot, c, 0:8, :] = turned[0:8]
        s_out[slot, c, 8:16, :] = turned[head_size : head_size + 8]

    def o_copy(c, slot, into, target):
        return remote(
            o_out.at[slot, :, cols(c)], o_in.at[into, :, cols(c)],
            o_ss.at[slot, c], o_rs.at[into, c], sp=target,
        )

    def s_copy(c, slot, into, target):
        return remote(
            s_out.at[slot, c], s_in.at[into, c], s_ss.at[slot, c], s_rs.at[into, c], sp=target
        )

    def give(c, slot, into, target):
        s_copy(c, slot, into, target).start()
        o_copy(c, slot, into, target).start()

    def early(c):
        @pl.when(c == chunks // 2)
        def _():
            relay("early")

    @pl.when(z == 0)
    def _():
        @pl.loop(0, chunks)
        def _(c):
            early(c)
            result, _lse = attend(c, q_own, [1], z, z, True)
            heads[:, cols(c)] = result.astype(heads.dtype)

    @pl.when(z == HUB)
    def _():
        @pl.loop(0, chunks)
        def _(c):
            early(c)
            k_copy(c).wait_recv()
            v_copy(c).wait_recv()
            q_copy(c, 1, 0, HUB).wait_recv()
            put(c, 1, *attend(c, q_in.at[1], [0, 1], 0, HUB + 2, False))
            q_copy(c, 0, 0, HUB).wait_recv()
            put(c, 0, *attend(c, q_in.at[0], [0, 1], 0, HUB + 1, False))
            give(c, 1, 0, HUB + 2)
            result, _lse = attend(c, q_own, [0, 1], 0, z, True)
            heads[:, cols(c)] = result.astype(heads.dtype)
            give(c, 0, 0, HUB + 1)

    @pl.when(z > HUB)
    def _():
        @pl.loop(0, chunks)
        def _(c):
            early(c)

            @pl.when(z == HUB + 1)
            def _():
                q_copy(c, 1, 1, HUB + 1).wait_recv()
                put(c, 1, *attend(c, q_in.at[1], [1], z, HUB + 2, False))

            result, lse = attend(c, q_own, [1], z, z, True)
            o_own[:, cols(c)] = result
            s_own[:, cols(c)] = lse

            @pl.when(z == HUB + 1)
            def _():
                give(c, 1, 1, HUB + 2)

    def taken(c, into):
        s_copy(c, 0, into, HUB).wait_recv()
        o_copy(c, 0, into, HUB).wait_recv()
        turned = s_in[into, c].T
        even = lax.broadcasted_iota(jnp.int32, (rows, LANES), 1) < head_size
        lse = jnp.where(even, turned[:, 0:1], turned[:, 8:9])
        return o_in[into, :, cols(c)].astype(jnp.float32), lse

    def merge(first, second):
        (a, la), (b, lb) = first, second
        top = jnp.maximum(la, lb)
        wa, wb = jnp.exp(la - top), jnp.exp(lb - top)
        total = wa + wb
        return (a * wa + b * wb) / total, top + jnp.log(total)

    @pl.when(z <= HUB)
    def _():
        relay("middle")

    @pl.when(z > HUB)
    def _():
        @pl.loop(0, chunks)
        def _(c):
            @pl.when(c == chunks // 2 + 1)
            def _():
                relay("middle")

            @pl.when(z == HUB + 2)
            def _():
                result, lse = merge((o_own[:, cols(c)], s_own[:, cols(c)]), taken(c, 1))
                o_own[:, cols(c)] = result
                s_own[:, cols(c)] = lse

            result, _lse = merge((o_own[:, cols(c)], s_own[:, cols(c)]), taken(c, 0))
            heads[:, cols(c)] = result.astype(heads.dtype)

        relay("late")

    width = w_buf.shape[2]

    def project(slot):
        owner = d
        for bit in (1, 2, 4):
            if slot & bit:
                owner = flip(owner, bit)
        block = jnp.dot(heads[...], w_buf[slot], preferred_element_type=jnp.float32)
        out_ref[0, :, pl.ds(pl.multiple_of(owner * width, LANES), width)] = block.astype(
            out_ref.dtype
        )

    project(0)
    for part in range(2):
        w_arrived(1, part)
    project(1)
    project(2)
    project(4)
    for slot in (3, 5):
        for part in range(2):
            w_arrived(slot, part)
        project(slot)

    @pl.when(z <= HUB)
    def _():
        relay("late")

    project(6)
    for part in range(2):
        w_arrived(7, part)
    project(7)

    gate_sends(lambda copy: copy.wait_send())
    for owner, target, relayed in ((0, 2, 0), (2, 0, 0), (1, 3, 0), (3, 1, 0), (0, 3, 1), (3, 0, 1)):
        @pl.when(z == (HUB if relayed else owner))
        def _():
            gate_copy(owner, target, relayed).wait_send()

    for stage in w_plan.values():
        for entry in stage:
            w_copy(*entry).wait_send()

    @pl.when(z == 0)
    def _():
        for c in range(chunks):
            k_copy(c).wait_send()
            v_copy(c).wait_send()

    @pl.when(z > HUB)
    def _():
        for c in range(chunks):
            q_copy(c, 0, 0, HUB).wait_send()

    @pl.when(z == HUB + 2)
    def _():
        for c in range(chunks):
            q_copy(c, 1, 1, HUB + 1).wait_send()

    @pl.when((z == HUB) | (z == HUB + 1))
    def _():
        for c in range(chunks):
            s_copy(c, 1, 0, HUB + 2).wait_send()
            o_copy(c, 1, 0, HUB + 2).wait_send()

    @pl.when(z == HUB)
    def _():
        for c in range(chunks):
            s_copy(c, 0, 0, HUB + 1).wait_send()
            o_copy(c, 0, 0, HUB + 1).wait_send()


def fused_shards(sp, queries, keys, values, cum_gates, out_weight):
    _, rows, width = queries.shape
    _, per, length = cum_gates.shape
    head_size = width // (per * sp)
    depth, block = out_weight.shape
    dp = 8
    chunks = width // LANES
    bf16, f32 = queries.dtype, jnp.float32
    dma = pltpu.SemaphoreType.DMA
    return pl.pallas_call(
        functools.partial(layer_kernel, (sp, chunks, head_size, head_size ** (-0.5))),
        out_shape=jax.ShapeDtypeStruct((1, rows, block * dp), bf16),
        in_specs=[pl.BlockSpec(memory_space=pltpu.HBM)] * 5,
        out_specs=pl.BlockSpec(memory_space=pltpu.VMEM),
        scratch_shapes=[
            pltpu.VMEM((rows, width), bf16),
            pltpu.VMEM((2, rows, width), bf16),
            pltpu.VMEM((2, rows, width), bf16),
            pltpu.VMEM((2, rows, width), bf16),
            pltpu.VMEM((sp, per, length), f32),
            pltpu.VMEM((chunks, 16, length), f32),
            pltpu.VMEM((2, rows, width), bf16),
            pltpu.VMEM((2, chunks, 16, LANES), f32),
            pltpu.VMEM((2, rows, width), bf16),
            pltpu.VMEM((2, chunks, 16, LANES), f32),
            pltpu.VMEM((rows, width), f32),
            pltpu.VMEM((rows, width), f32),
            pltpu.VMEM((rows, width), bf16),
            pltpu.VMEM((dp, depth, block), bf16),
            dma((2, chunks)), dma((2, chunks)), dma((2, chunks)), dma((2, chunks)),
            dma((2, chunks)), dma((2, chunks)), dma((2, chunks)), dma((2, chunks)),
            dma((2, sp)), dma((sp,)), dma((14,)), dma((dp, 2)), dma((5,)),
            pltpu.SemaphoreType.REGULAR((2,)),
        ],
        compiler_params=pltpu.CompilerParams(collective_id=0, has_side_effects=True, vmem_limit_bytes=16 * 2**20),
        name="layer",
    )(*(pltpu.with_memory_space_constraint(x, pltpu.HBM) for x in (queries, keys, values, cum_gates, out_weight)))


def route(sp, dp, queries, keys, values, cum_gates, out_weight):
    _, rows, width = queries.shape
    head_size = width // (cum_gates.shape[1] * sp)
    fits = (
        sp == HUB + 3
        and dp == 8
        and rows == LANES
        and 2 * head_size == LANES
        and width % LANES == 0
        and out_weight.shape[1] % LANES == 0
    )
    if fits:
        return fused_shards(sp, queries, keys, values, cum_gates, out_weight)
    return shards(queries, keys, values, cum_gates, out_weight)


def solution(mesh):
    in_specs = (
        P("dp", "sp", None),
        P("dp", "sp", None),
        P("dp", "sp", None),
        P("dp", "sp", None),
        P(None, "dp"),
    )
    out_specs = P("dp", "sp", None)
    body = functools.partial(route, mesh.shape["sp"], mesh.shape["dp"])
    return jax.shard_map(body, mesh=mesh, in_specs=in_specs, out_specs=out_specs, check_vma=False)
```
